32 devices in a mesh: ep: 8 (over z, core), tp: 4 (over y, x).
Axes of the slice: x: 2, y: 2, z: 4, core: 2. Of those that a mesh axis runs over, the one named last changes fastest.
Arguments:
- tokens: bfloat16 [256, 2048], P('ep'), may hold values from -6 to 6
- recurrent_head_state: float32 [256, 16, 4096], P('ep', 'tp'), may hold values from -4 to 4
- first_norm_gain: float32 [2048], replicated, may hold values from 0.1 to 1.9
- receptance_matrix: bfloat16 [2048, 1024], P(None, 'tp'), may hold values from -0.125 to 0.125
- key_matrix: bfloat16 [2048, 1024], P(None, 'tp'), may hold values from -0.125 to 0.125
- value_matrix: bfloat16 [2048, 1024], P(None, 'tp'), may hold values from -0.125 to 0.125
- decay_matrix: bfloat16 [2048, 1024], P(None, 'tp'), may hold values from -0.125 to 0.125
- decay_offset: float32 [1024], P('tp'), may hold values from -3 to 0.5
- correction_offset: float32 [1024], P('tp'), may hold values from -2 to 2
- correction_key_factor: float32 [1024], P('tp'), may hold values from -1 to 1
- own_term_weight: float32 [1024], P('tp'), may hold values from -0.9 to 0.9
- head_norm_gain: float32 [1024], P('tp'), may hold values from 0.1 to 1.9
- output_matrix: bfloat16 [1024, 2048], P('tp'), may hold values from -0.1875 to 0.1875
- second_norm_gain: float32 [2048], replicated, may hold values from 0.1 to 1.9
- routing: int32 [256, 2], replicated, may hold values from 0 to 7, all different within a row; in each aligned block of 32 rows (0 to 31, 32 to 63, ...) at most 16 rows name the same one
- routing_weight: float32 [256, 2], P('ep'), may hold values from 0.1 to 1
- expert_gate_weight: bfloat16 [8, 2048, 4096], P('ep', None, 'tp'), may hold values from -0.125 to 0.125
- expert_up_weight: bfloat16 [8, 2048, 4096], P('ep', None, 'tp'), may hold values from -0.125 to 0.125
- expert_down_weight: bfloat16 [8, 4096, 2048], P('ep', 'tp'), may hold values from -0.125 to 0.125
- dense_gate_weight: bfloat16 [2048, 2816], P(None, 'ep'), may hold values from -0.125 to 0.125
- dense_up_weight: bfloat16 [2048, 2816], P(None, 'ep'), may hold values from -0.125 to 0.125
- dense_down_weight: bfloat16 [2816, 2048], P('ep'), may hold values from -0.109375 to 0.109375
- dense_gate_offset: float32 [2048], replicated, may hold values from -3 to 3
Outputs:
- layer_out: bfloat16 [256, 2048], P(('ep', 'tp'))
- next_state: float32 [256, 16, 4096], P('ep', 'tp')
The draws below stay inside these ranges and needn't reach their ends.
Inputs may be any that keep to these rules, and one draw needn't show every extreme that they name: `routing`: each row names 2 different experts. In each aligned block of 32 rows no expert is named more than 16 times, a bound that some block reaches.
All inputs are finite; a program needn't handle non-finite values.
Results may differ from the reference program's by a relative error of at most 0.017.
Values may be sent and summed in bfloat16 or wider, within the bound.
No kernel may reach another device: no remote copies, remote signals or barrier semaphores. Data moves between devices by JAX's collectives and lax.ppermute only.
A program may use at most 64 MiB of HBM per device.

```python
import math
from functools import partial
import jax
import jax.numpy as jnp
import numpy as np
from jax import lax

D = 2048
HEAD_COUNT = 16
HEAD_WIDTH = 64
FF_E = 4096
FF_D = 2816
TOP_K = 2
B_DEV = 32
B_TOT = 256
EXPERTS = 8
CAP = 16
N_EP = 8


def strengthened(entries, rng, source, target, parts, factor):
    def block_of(axis_at):
        return (jnp.arange(entries.shape[axis_at]) // (entries.shape[axis_at] // parts)).reshape((-1,) + (1,) * (entries.ndim - 1 - axis_at))

    first = jax.random.permutation(rng, parts)[block_of(target)]
    second = (block_of(target) + parts // 2) % parts
    return jnp.where((block_of(source) == first) | (block_of(source) == second), factor * entries, entries)


def levels(rng, extent, pieces, smallest, high):
    level, own = 1.0, jax.random.fold_in(rng, 6)
    for position, blocks in pieces:
        draws = jnp.exp(jax.random.uniform(jax.random.fold_in(own, position), (blocks,), jnp.float32, smallest / len(pieces), high / len(pieces)))
        level = level * jnp.repeat(draws, extent[position] // blocks).reshape([-1 if axis == position else 1 for axis in range(len(extent))])
    return level


def shared_out(stream_key, own, number, rows, amount, top, most, lean):
    sequence = jax.random.permutation(stream_key, amount)
    crowded, common = shares(amount, rows * top, most, lean, True), shares(amount, rows * top, most, lean, False)
    places = jnp.arange(amount)

    def named(tallies, turn):
        used = int((tallies > 0).sum())
        fixed = max(1, used // 4)
        moved = fixed + (places - fixed + turn * (used - fixed)) % max(1, amount - fixed)
        return jnp.zeros((amount,), jnp.int32).at[sequence[jnp.where(places < fixed, places, moved)]].set(jnp.asarray(tallies, jnp.int32))

    tallies = jnp.where(number % 4 == 0, named(crowded, number // 4), named(common, number - number // 4 - 1))
    mixed = jax.random.permutation(jax.random.fold_in(own, 3), amount)
    giver, receiver = mixed[0:amount // 2 * 2:2], mixed[1:amount // 2 * 2:2]
    room = jnp.minimum(tallies[giver] - 1, most - tallies[receiver]) // 2
    room = jnp.where((giver == sequence[0]) | (receiver == sequence[0]) | (tallies[receiver] == 0), 0, jnp.maximum(room, 0))
    moved = jax.random.randint(jax.random.fold_in(own, 4), (amount // 2,), 0, 1 << 20) % (room + 1)
    tallies = tallies.at[giver].add(-moved).at[receiver].add(moved)
    labels = jnp.searchsorted(jnp.cumsum(tallies), jnp.arange(rows * top), side="right").astype(jnp.int32)
    listing = labels.reshape(top, rows).T
    listing = listing[jax.random.permutation(jax.random.fold_in(own, 1), rows)]
    turn = jax.random.randint(jax.random.fold_in(own, 2), (rows, 1), 0, top)
    return jnp.take_along_axis(listing, (jnp.arange(top)[None, :] + turn) % top, axis=1)


def shares(amount, total, reach, slope, full):
    weights = [(1 << 20) // math.isqrt(grade ** slope) + 1 for grade in range(1, amount + 1)]
    largest = reach if full else min(reach, max(-(-total // amount), total * weights[0] // sum(weights)))
    least = 1 if total - largest >= amount - 1 else 0
    counts, spare = [largest] + [least] * (amount - 1), total - largest - least * (amount - 1)
    while spare > 0:
        movable = [i for i in range(1, amount) if counts[i] < largest] or [i for i in range(1, amount) if counts[i] < reach]
        pool, left = sum([weights[i] for i in movable]), spare
        for i in movable:
            extra = min(reach - counts[i], max(1, left * weights[i] // pool), spare)
            counts[i] = counts[i] + extra
            spare = spare - extra
    return np.array(counts)


def bell_draw(stream_key, dims, width, limit, split=(), kind=jnp.bfloat16):
    entries = jax.random.normal(stream_key, dims, jnp.float32) * width
    if len(split) > 0:
        entries = levels(stream_key, dims, split, -0.22, 0.18) * entries
    return jnp.clip(entries, min=-limit, max=limit).astype(kind)


def gaussian_with(rng, dims, scale, limit, pieces, heavy, kind=jnp.bfloat16):
    drawn = scale * jax.random.normal(rng, dims, jnp.float32)
    if pieces:
        drawn = drawn * levels(rng, dims, pieces, -0.22, 0.18)
    return jnp.clip(strengthened(drawn, jax.random.fold_in(rng, 3), *heavy), -limit, limit).astype(kind)


def setup_inputs(seed: int = 0) -> dict:
    streams_of = jax.random.split(jax.random.key(seed), 24)
    tokens = bell_draw(streams_of[0], (B_TOT, D), 1.0, 6.0, ((0, 8),))
    recurrent_head_state = bell_draw(streams_of[1], (B_TOT, HEAD_COUNT, HEAD_WIDTH * HEAD_WIDTH), 0.5, 4.0, ((0, 8), (1, 4)), jnp.float32)
    first_norm_gain = jnp.clip(1.0 + 0.18 * jax.random.normal(streams_of[2], (D,), jnp.float32), 0.1, 1.9)
    receptance_matrix = bell_draw(streams_of[3], (D, HEAD_COUNT * HEAD_WIDTH), D ** -0.5, 0.125, ((1, 4),))
    key_matrix = bell_draw(streams_of[4], (D, HEAD_COUNT * HEAD_WIDTH), D ** -0.5, 0.125, ((1, 4),))
    value_matrix = bell_draw(streams_of[5], (D, HEAD_COUNT * HEAD_WIDTH), D ** -0.5, 0.125, ((1, 4),))
    decay_matrix = bell_draw(streams_of[6], (D, HEAD_COUNT * HEAD_WIDTH), D ** -0.5, 0.125, ((1, 4),))
    decay_offset = jnp.clip(-3.0 + 3.5 * jax.random.uniform(streams_of[7], (HEAD_COUNT * HEAD_WIDTH,), jnp.float32) ** levels(streams_of[7], (HEAD_COUNT * HEAD_WIDTH,), ((0, 4),), -0.2, 0.2), -3.0, 0.5)
    correction_offset = jnp.clip(jax.random.uniform(streams_of[8], (HEAD_COUNT * HEAD_WIDTH,), jnp.float32, -2.0, 2.0) * levels(streams_of[8], (HEAD_COUNT * HEAD_WIDTH,), ((0, 4),), -0.4, 0.0), -2.0, 2.0)
    correction_key_factor = jnp.clip(jax.random.uniform(streams_of[9], (HEAD_COUNT * HEAD_WIDTH,), jnp.float32, -1.0, 1.0) * levels(streams_of[9], (HEAD_COUNT * HEAD_WIDTH,), ((0, 4),), -0.4, 0.0), -1.0, 1.0)
    own_term_weight = bell_draw(streams_of[10], (HEAD_COUNT * HEAD_WIDTH,), 0.15, 0.9, ((0, 4),), jnp.float32)
    head_norm_gain = jnp.clip(1.0 + 0.18 * jax.random.normal(streams_of[11], (HEAD_COUNT * HEAD_WIDTH,), jnp.float32), 0.1, 1.9)
    output_matrix = bell_draw(streams_of[12], (HEAD_COUNT * HEAD_WIDTH, D), (HEAD_COUNT * HEAD_WIDTH) ** -0.5, 0.1875, ((0, 4),))
    second_norm_gain = jnp.clip(1.0 + 0.18 * jax.random.normal(streams_of[13], (D,), jnp.float32), 0.1, 1.9)
    routing_keys = jax.random.split(jax.random.fold_in(streams_of[14], 1), B_TOT // B_DEV)
    routing_turns = jax.random.permutation(jax.random.fold_in(streams_of[14], 3), B_TOT // B_DEV)
    routing = jax.vmap(lambda own, number: shared_out(jax.random.fold_in(streams_of[14], 2), own, number, B_DEV, EXPERTS, TOP_K, CAP, 2))(routing_keys, routing_turns).reshape((B_TOT, TOP_K))
    routing_weight = jnp.clip(0.1 + 0.9 * jax.random.uniform(streams_of[15], (B_TOT, TOP_K), jnp.float32) ** levels(streams_of[15], (B_TOT, TOP_K), ((0, 8),), -0.2, 0.2), 0.1, 1.0)
    expert_gate_weight = bell_draw(streams_of[16], (EXPERTS, D, FF_E), D ** -0.5, 0.125, ((0, 8), (2, 4)))
    expert_up_weight = bell_draw(streams_of[17], (EXPERTS, D, FF_E), D ** -0.5, 0.125, ((0, 8), (2, 4)))
    expert_down_weight = gaussian_with(streams_of[18], (EXPERTS, FF_E, D), FF_E ** -0.5, 0.125, ((0, 8), (1, 4)), (1, 2, 4, 2.0))
    dense_gate_weight = bell_draw(streams_of[19], (D, FF_D), D ** -0.5, 0.125, ((1, 8),))
    dense_up_weight = bell_draw(streams_of[20], (D, FF_D), D ** -0.5, 0.125, ((1, 8),))
    dense_down_weight = bell_draw(streams_of[21], (FF_D, D), FF_D ** -0.5, 0.109375, ((0, 8),))
    dense_gate_offset = jnp.clip(jax.random.uniform(streams_of[22], (D,), jnp.float32, -3.0, 3.0), -3.0, 3.0)
    return {"tokens": tokens, "recurrent_head_state": recurrent_head_state, "first_norm_gain": first_norm_gain, "receptance_matrix": receptance_matrix, "key_matrix": key_matrix, "value_matrix": value_matrix, "decay_matrix": decay_matrix, "decay_offset": decay_offset, "correction_offset": correction_offset, "correction_key_factor": correction_key_factor, "own_term_weight": own_term_weight, "head_norm_gain": head_norm_gain, "output_matrix": output_matrix, "second_norm_gain": second_norm_gain, "routing": routing, "routing_weight": routing_weight, "expert_gate_weight": expert_gate_weight, "expert_up_weight": expert_up_weight, "expert_down_weight": expert_down_weight, "dense_gate_weight": dense_gate_weight, "dense_up_weight": dense_up_weight, "dense_down_weight": dense_down_weight, "dense_gate_offset": dense_gate_offset}


PRECISE = lax.Precision.HIGHEST

def rms_scale(rows, gain):
    floats = rows.astype(jnp.float32)
    return floats * lax.rsqrt(lax.optimization_barrier(jnp.mean(floats * floats, axis=-1, keepdims=True)) + 1e-06) * gain

def route_table(block_routes, experts, capacity):
    flat_routes = block_routes.reshape(-1)
    chosen = (flat_routes[:, None] == jnp.arange(experts, dtype=jnp.int32)[None, :]).astype(jnp.int32)
    before = jnp.cumsum(chosen, axis=0, dtype=jnp.int32) - chosen
    slot_index = lax.optimization_barrier(jnp.sum(before * chosen, axis=1))
    slot_match = (slot_index[:, None] == jnp.arange(capacity, dtype=jnp.int32)[None, :]).astype(jnp.float32)
    dispatch_table = chosen.astype(jnp.float32)[:, :, None] * slot_match[:, None, :]
    return dispatch_table.reshape(block_routes.shape[0], block_routes.shape[1], experts, capacity)

def state_update(receptance_rows, key_matrix_rows, value_matrix_rows, decay_logits, recurrent_head_state, decay_offset, correction_offset, correction_key_factor, own_term_weight, head_norm_gain, head_width):
    seq_count = key_matrix_rows.shape[0]
    decay_factor = jnp.exp(-jnp.exp(decay_offset + decay_logits))
    in_rate = jax.nn.sigmoid(correction_offset + correction_key_factor * key_matrix_rows)
    key_in = key_matrix_rows * in_rate

    def split_heads(block):
        return block.reshape(seq_count, -1, head_width)
    keys_head = split_heads(key_matrix_rows)
    unit_keys = keys_head * lax.rsqrt(lax.optimization_barrier(jnp.mean(keys_head * keys_head, axis=-1, keepdims=True)) + 1e-06) * head_width ** (-0.5)
    rate_head = split_heads(in_rate)
    head_keys = split_heads(key_in)
    decay_head = split_heads(decay_factor)
    head_values = split_heads(value_matrix_rows)
    head_receptance = split_heads(receptance_rows)
    matrix = recurrent_head_state.reshape(seq_count, -1, head_width, head_width)
    removed = jnp.einsum('bhvk,bhk->bhv', matrix, unit_keys, precision=PRECISE)
    updated = matrix * decay_head[:, :, None, :] - removed[..., None] * (unit_keys * rate_head)[:, :, None, :] + head_values[..., None] * head_keys[:, :, None, :]
    readout = jnp.einsum('bhvk,bhk->bhv', updated, head_receptance, precision=PRECISE)
    center = lax.optimization_barrier(jnp.mean(readout, axis=-1, keepdims=True))
    spread = lax.optimization_barrier(jnp.mean(jnp.square(readout - center), axis=-1, keepdims=True))
    normalized_rows = (readout - center) * lax.rsqrt(spread + 0.00064) * head_norm_gain.reshape(-1, head_width)
    own_term_total = lax.optimization_barrier(jnp.sum(head_receptance * head_keys * own_term_weight.reshape(-1, head_width), axis=-1, keepdims=True))
    normalized_rows = normalized_rows + own_term_total * head_values
    return (normalized_rows.reshape(seq_count, -1).astype(jnp.bfloat16), updated.reshape(seq_count, -1, head_width * head_width))

def reference(tokens, recurrent_head_state, first_norm_gain, receptance_matrix, key_matrix, value_matrix, decay_matrix, decay_offset, correction_offset, correction_key_factor, own_term_weight, head_norm_gain, output_matrix, second_norm_gain, routing, routing_weight, expert_gate_weight, expert_up_weight, expert_down_weight, dense_gate_weight, dense_up_weight, dense_down_weight, dense_gate_offset):
    normalized_rows = rms_scale(tokens, first_norm_gain).astype(jnp.bfloat16)
    receptance_rows = jnp.dot(normalized_rows, receptance_matrix, preferred_element_type=jnp.float32)
    key_matrix_rows = jnp.dot(normalized_rows, key_matrix, preferred_element_type=jnp.float32)
    value_matrix_rows = jnp.dot(normalized_rows, value_matrix, preferred_element_type=jnp.float32)
    decay_logits = jnp.dot(normalized_rows, decay_matrix, preferred_element_type=jnp.float32)
    head_outputs, next_state = state_update(receptance_rows, key_matrix_rows, value_matrix_rows, decay_logits, recurrent_head_state, decay_offset, correction_offset, correction_key_factor, own_term_weight, head_norm_gain, HEAD_WIDTH)
    hidden_sum = tokens.astype(jnp.float32) + jnp.dot(head_outputs, output_matrix, preferred_element_type=jnp.float32)
    ffn_in = rms_scale(hidden_sum, second_norm_gain).astype(jnp.bfloat16)
    tables = jax.vmap(partial(route_table, experts=EXPERTS, capacity=CAP))(routing.reshape(N_EP, B_DEV, TOP_K))
    grouped = ffn_in.reshape(N_EP, B_DEV, D).astype(jnp.float32)
    buffers = jnp.einsum('sbkec,sbd->escd', tables, grouped, precision=PRECISE).astype(jnp.bfloat16)

    def one_expert(packed):
        rows, gate_part, up_part, down_part = packed
        flat_rows = rows.reshape(-1, D)
        gate_pre = jnp.dot(flat_rows, gate_part, preferred_element_type=jnp.float32)
        up_pre = jnp.dot(flat_rows, up_part, preferred_element_type=jnp.float32)
        hidden = (jax.nn.silu(gate_pre) * up_pre).astype(jnp.bfloat16)
        result = jnp.dot(hidden, down_part, preferred_element_type=jnp.float32).astype(jnp.bfloat16)
        return result.reshape(rows.shape)
    expert_outs = lax.map(one_expert, (buffers, expert_gate_weight, expert_up_weight, expert_down_weight))
    weighted = jnp.einsum('sbkec,sbk->secb', tables, routing_weight.reshape(N_EP, B_DEV, TOP_K), precision=PRECISE)
    moe = jnp.einsum('secb,escd->sbd', weighted, expert_outs.astype(jnp.float32), precision=PRECISE).reshape(B_TOT, D)
    dense_hidden = (jax.nn.silu(jnp.dot(ffn_in, dense_gate_weight, preferred_element_type=jnp.float32)) * jnp.dot(ffn_in, dense_up_weight, preferred_element_type=jnp.float32)).astype(jnp.bfloat16)
    block_units = FF_D // N_EP

    def add_block(total, index):
        start = index * block_units
        piece = lax.dynamic_slice_in_dim(dense_hidden, start, block_units, 1)
        rows = lax.dynamic_slice_in_dim(dense_down_weight, start, block_units, 0)
        part = jnp.dot(piece, rows, preferred_element_type=jnp.float32).astype(jnp.bfloat16)
        part = lax.optimization_barrier(part)
        return (total + part.astype(jnp.float32), None)
    dense_sum, _ = lax.scan(add_block, jnp.zeros((B_TOT, D), jnp.float32), jnp.arange(N_EP, dtype=jnp.int32))
    layer_out = (hidden_sum + moe + jax.nn.sigmoid(dense_gate_offset) * dense_sum).astype(jnp.bfloat16)
    return (layer_out, next_state)
```

```python
import functools

import jax
import jax.numpy as jnp
from jax import lax
from jax.experimental import pallas as pl
from jax.experimental.pallas import tpu as pltpu
from jax.sharding import PartitionSpec as P

HEAD_WIDTH = 64
F32 = jnp.float32
BF16 = jnp.bfloat16
HIGHEST = lax.Precision.HIGHEST
VMEM = pl.BlockSpec(memory_space=pltpu.VMEM)
SMEM = pl.BlockSpec(memory_space=pltpu.SMEM)


def iota(shape, dim):
    return lax.broadcasted_iota(jnp.int32, shape, dim)


def dot(a, b):
    return jnp.dot(a, b, preferred_element_type=F32)


def dot_exact(a, b):
    return jnp.dot(a, b, preferred_element_type=F32, precision=HIGHEST)


def halves(x):
    high = x.astype(BF16)
    return high, (x - high.astype(F32)).astype(BF16)


def rms_rows(floats, gain):
    return floats * lax.rsqrt(jnp.mean(floats * floats, axis=-1, keepdims=True) + 1e-06) * gain


def silu(x):
    return x * jax.nn.sigmoid(x)


def attention_kernel(
    tokens,
    state,
    gain,
    rec_m,
    key_m,
    val_m,
    dec_m,
    dec_off,
    cor_off,
    cor_fac,
    own_w,
    head_gain,
    out_m,
    next_state,
    partial,
    rows_ref,
):
    seqs, heads, area = state.shape
    width = area // HEAD_WIDTH
    count = seqs * heads
    for b in range(seqs):
        rows_ref[b * heads : (b + 1) * heads, :] = state[b]
    normed = rms_rows(tokens[...].astype(F32), gain[...]).astype(BF16)
    rec = dot(normed, rec_m[...])
    keys = dot(normed, key_m[...])
    vals = dot(normed, val_m[...])
    decay = jnp.exp(-jnp.exp(dec_off[...] + dot(normed, dec_m[...])))
    rate = jax.nn.sigmoid(cor_off[...] + cor_fac[...] * keys)
    key_in = keys * rate

    def by_head(x):
        return jnp.concatenate([x[:, h * width : (h + 1) * width] for h in range(heads)], axis=0)

    keys_h = by_head(keys)
    unit = (
        keys_h
        * lax.rsqrt(jnp.mean(keys_h * keys_h, axis=-1, keepdims=True) + 1e-06)
        * width ** (-0.5)
    )
    erase = unit * by_head(rate)
    rec_h = by_head(rec)
    key_in_h = by_head(key_in)
    vals_h = by_head(vals)
    decay_h = by_head(decay)
    own = jnp.sum(by_head(rec * key_in * own_w[...]), axis=-1, keepdims=True)
    erase_dot = jnp.sum(erase * rec_h, axis=-1, keepdims=True)
    write_dot = jnp.sum(key_in_h * rec_h, axis=-1, keepdims=True)
    row = iota((count, count), 0)
    col = iota((count, count), 1)
    to_seq = (col == (row % heads) * seqs + row // heads).astype(F32)
    to_head = (row == (col % heads) * seqs + col // heads).astype(F32)
    packed = dot_exact(
        to_seq,
        jnp.concatenate([unit, decay_h * rec_h, decay_h, erase, key_in_h, vals_h], axis=1),
    )

    def twice(n):
        part = packed[:, n * width : (n + 1) * width]
        return jnp.concatenate([part, part], axis=1)

    chunk = 8 * width
    steps = area // chunk

    def wide(n):
        return jnp.concatenate([twice(n)] * (chunk // (2 * width)), axis=1)

    unit_w = wide(0)
    read_w = wide(1)
    sums = jnp.zeros((count, 2 * width), F32)
    lane = iota((chunk, 2 * width), 0) // width
    slot = iota((chunk, 2 * width), 1)
    for j in range(steps):
        block = rows_ref[:, j * chunk : (j + 1) * chunk]
        left = (slot == lane + 8 * j).astype(F32).astype(BF16)
        right = (slot == lane + (8 * j + width)).astype(F32).astype(BF16)
        a_hi, a_lo = halves(block * unit_w)
        b_hi, b_lo = halves(block * read_w)
        sums = sums + (dot(a_hi, left) + dot(a_lo, left)) + (dot(b_hi, right) + dot(b_lo, right))
    removed_hi, removed_lo = halves(sums[:, :width])
    removed_x = jnp.concatenate([removed_hi, removed_lo], axis=1)
    vals_hi, vals_lo = halves(packed[:, 5 * width : 6 * width])
    vals_x = jnp.concatenate([vals_hi, vals_lo], axis=1)
    decay_w = wide(2)
    erase_w = wide(3)
    key_w = wide(4)
    source = iota((2 * width, chunk), 0) % width
    target = iota((2 * width, chunk), 1) // width
    for j in range(steps):
        spread = (source == target + 8 * j).astype(F32).astype(BF16)
        block = rows_ref[:, j * chunk : (j + 1) * chunk]
        rows_ref[:, j * chunk : (j + 1) * chunk] = (
            block * decay_w - dot(removed_x, spread) * erase_w + dot(vals_x, spread) * key_w
        )
    for b in range(seqs):
        next_state[b] = rows_ref[b * heads : (b + 1) * heads, :]
    sums_h = dot_exact(to_head, sums)
    read = sums_h[:, width:] - sums_h[:, :width] * erase_dot + vals_h * write_dot
    center = jnp.mean(read, axis=-1, keepdims=True)
    shifted = read - center
    spread_sq = jnp.mean(shifted * shifted, axis=-1, keepdims=True)
    normal = shifted * lax.rsqrt(spread_sq + 0.00064)
    extra = own * vals_h

    def by_lane(x):
        return jnp.concatenate([x[h * seqs : (h + 1) * seqs] for h in range(heads)], axis=1)

    heads_out = (by_lane(normal) * head_gain[...] + by_lane(extra)).astype(BF16)
    partial[...] = dot(heads_out, out_m[...]).astype(BF16)


def dispatch_kernel(
    place, parts, tokens, gain, routing, weights, own_hidden, own_rows, table, *sends
):
    seqs, _ = tokens.shape
    groups = len(sends)
    capacity = sends[0].shape[0]
    per_lane = own_rows.shape[0]
    me = place[0]
    lane = place[1]
    hidden = tokens[...].astype(F32)
    total = parts[0].astype(F32)
    for n in range(1, parts.shape[0]):
        total = total + parts[n].astype(F32)
    hidden = hidden + total
    rows = rms_rows(hidden, gain[...]).astype(BF16)
    slots = groups * capacity
    col = iota((seqs, slots), 1)
    expert = (col // capacity) ^ me
    place_in = (col % capacity).astype(F32)
    routes = routing[pl.ds(pl.multiple_of(me * seqs, seqs), seqs), :]
    chosen = jnp.zeros((seqs, slots), F32)
    weighted = jnp.zeros((seqs, slots), F32)
    for k in range(routing.shape[1]):
        hit = (routes[:, k : k + 1] == expert).astype(F32)
        chosen = chosen + hit
        weighted = weighted + hit * weights[:, k : k + 1]
    earlier = (iota((seqs, seqs), 1) < iota((seqs, seqs), 0)).astype(F32).astype(BF16)
    before = dot(earlier, chosen.astype(BF16))
    here = (before == place_in).astype(F32)
    pick = jnp.transpose(chosen * here).astype(BF16)
    sent = dot(pick, rows).astype(BF16)
    for k in range(groups):
        sends[k][...] = sent[k * capacity : (k + 1) * capacity]
    row = iota((seqs, seqs), 0)
    shuffled = ((row // per_lane) ^ lane) * per_lane + row % per_lane
    order = (iota((seqs, seqs), 1) == shuffled).astype(F32)
    table[...] = dot_exact(order, weighted * here)
    mine = order[:per_lane]
    own_hidden[...] = dot_exact(mine, hidden)
    own_rows[...] = dot(mine.astype(BF16), rows).astype(BF16)


def dense_kernel(groups, *refs):
    rows = refs[:groups]
    gate, up, down = refs[groups : groups + 3]
    outs = refs[groups + 3 : 2 * groups + 3]
    gathered = refs[-1]
    per = rows[0].shape[0]
    for k in range(groups):
        gathered[k * per : (k + 1) * per, :] = rows[k][...].astype(F32)
    x = gathered[...].astype(BF16)
    hidden = (silu(dot(x, gate[...])) * dot(x, up[...])).astype(BF16)
    result = dot(hidden, down[...])
    for k in range(groups):
        outs[k][...] = result[k * per : (k + 1) * per].astype(BF16)


def expert_kernel(groups, *refs):
    rows = refs[:groups]
    gate, up, down = refs[groups : groups + 3]
    outs = refs[groups + 3 : 2 * groups + 3]
    gathered, total = refs[-2:]
    per = rows[0].shape[0]
    step = pl.program_id(0)

    @pl.when(step == 0)
    def _():
        for k in range(groups):
            gathered[k * per : (k + 1) * per, :] = rows[k][...].astype(F32)
        total[...] = jnp.zeros_like(total)

    x = gathered[...].astype(BF16)
    hidden = (silu(dot(x, gate[0])) * dot(x, up[0])).astype(BF16)
    total[...] += dot(hidden, down[0])

    @pl.when(step == pl.num_programs(0) - 1)
    def _():
        for k in range(groups):
            outs[k][...] = total[k * per : (k + 1) * per].astype(BF16)


def combine_kernel(groups, table, *refs):
    rows = refs[:groups]
    own = refs[groups]
    sends = refs[groups + 1 : -1]
    gathered = refs[-1]
    per = rows[0].shape[0]
    per_lane = own.shape[0]
    for k in range(groups):
        gathered[k * per : (k + 1) * per, :] = rows[k][...].astype(F32)
    x = gathered[...].astype(BF16)
    high, low = halves(table[...])
    result = dot(high, x) + dot(low, x)
    own[...] = result[:per_lane]
    for k in range(len(sends)):
        sends[k][...] = result[(k + 1) * per_lane : (k + 2) * per_lane].astype(BF16)


def final_kernel(groups, hidden, moe, offset, *refs):
    dense = refs[:groups]
    others = refs[groups:-1]
    out = refs[-1]
    block = dense[0][...].astype(F32)
    for k in range(1, groups):
        block = block + dense[k][...].astype(F32)
    total = moe[...]
    for other in others:
        total = total + other[...].astype(F32)
    out[...] = (hidden[...] + total + jax.nn.sigmoid(offset[...]) * block).astype(BF16)


def like(shape, dtype):
    return jax.ShapeDtypeStruct(shape, dtype)


def exchange(arrays, axis):
    size = lax.axis_size(axis)
    return [arrays[0]] + [
        lax.ppermute(arrays[k], axis, [(i, i ^ k) for i in range(size)]) for k in range(1, size)
    ]


def local(
    tokens,
    recurrent_head_state,
    first_norm_gain,
    receptance_matrix,
    key_matrix,
    value_matrix,
    decay_matrix,
    decay_offset,
    correction_offset,
    correction_key_factor,
    own_term_weight,
    head_norm_gain,
    output_matrix,
    second_norm_gain,
    routing,
    routing_weight,
    expert_gate_weight,
    expert_up_weight,
    expert_down_weight,
    dense_gate_weight,
    dense_up_weight,
    dense_down_weight,
    dense_gate_offset,
):
    seqs, width = tokens.shape
    heads, area = recurrent_head_state.shape[1:]
    groups = lax.axis_size("ep")
    lanes = lax.axis_size("tp")
    per_lane = seqs // lanes
    local_experts, _, units = expert_gate_weight.shape
    assert local_experts == 1
    capacity = 2 * seqs * routing.shape[1] // groups
    place = jnp.stack([lax.axis_index("ep"), lax.axis_index("tp")]).astype(jnp.int32)

    def row(x):
        return x.reshape(1, -1)

    next_state, partial = pl.pallas_call(
        attention_kernel,
        out_shape=(like(recurrent_head_state.shape, F32), like((seqs, width), BF16)),
        in_specs=[VMEM] * 13,
        out_specs=(VMEM, VMEM),
        scratch_shapes=[pltpu.VMEM((seqs * heads, area), F32)],
        name="attention",
    )(
        tokens,
        recurrent_head_state,
        row(first_norm_gain),
        receptance_matrix,
        key_matrix,
        value_matrix,
        decay_matrix,
        row(decay_offset),
        row(correction_offset),
        row(correction_key_factor),
        row(own_term_weight),
        row(head_norm_gain),
        output_matrix,
    )
    parts = lax.all_gather(partial, "tp", axis=0, tiled=False)
    own_hidden, own_rows, table, *sends = pl.pallas_call(
        dispatch_kernel,
        out_shape=(
            like((per_lane, width), F32),
            like((per_lane, width), BF16),
            like((seqs, groups * capacity), F32),
            *[like((capacity, width), BF16)] * groups,
        ),
        in_specs=[SMEM] + [VMEM] * 5,
        out_specs=[VMEM] * (3 + groups),
        name="dispatch",
    )(place, parts, tokens, row(second_norm_gain), routing, routing_weight)
    dense_in = exchange([own_rows] * groups, "ep")
    expert_in = exchange(sends, "ep")
    dense_out = pl.pallas_call(
        functools.partial(dense_kernel, groups),
        out_shape=[like((per_lane, width), BF16)] * groups,
        in_specs=[VMEM] * (groups + 3),
        out_specs=[VMEM] * groups,
        scratch_shapes=[pltpu.VMEM((groups * per_lane, width), F32)],
        name="dense",
    )(*dense_in, dense_gate_weight, dense_up_weight, dense_down_weight)
    dense_back = exchange(dense_out, "ep")
    tile = min(256, units)
    whole = pl.BlockSpec((capacity, width), lambda i: (0, 0))
    expert_out = pl.pallas_call(
        functools.partial(expert_kernel, groups),
        grid=(units // tile,),
        out_shape=[like((capacity, width), BF16)] * groups,
        in_specs=[whole] * groups
        + [
            pl.BlockSpec((1, width, tile), lambda i: (0, 0, i)),
            pl.BlockSpec((1, width, tile), lambda i: (0, 0, i)),
            pl.BlockSpec((1, tile, width), lambda i: (0, i, 0)),
        ],
        out_specs=[whole] * groups,
        scratch_shapes=[
            pltpu.VMEM((groups * capacity, width), F32),
            pltpu.VMEM((groups * capacity, width), F32),
        ],
        name="experts",
    )(*expert_in, expert_gate_weight, expert_up_weight, expert_down_weight)
    expert_back = exchange(expert_out, "ep")
    moe_own, *moe_sends = pl.pallas_call(
        functools.partial(combine_kernel, groups),
        out_shape=[like((per_lane, width), F32)] + [like((per_lane, width), BF16)] * (lanes - 1),
        in_specs=[VMEM] * (groups + 1),
        out_specs=[VMEM] * lanes,
        scratch_shapes=[pltpu.VMEM((groups * capacity, width), F32)],
        name="combine",
    )(table, *expert_back)
    moe_in = exchange([moe_own] + moe_sends, "tp")
    layer_out = pl.pallas_call(
        functools.partial(final_kernel, groups),
        out_shape=like((per_lane, width), BF16),
        in_specs=[VMEM] * (3 + groups + lanes - 1),
        out_specs=VMEM,
        name="final",
    )(own_hidden, moe_in[0], row(dense_gate_offset), *dense_back, *moe_in[1:])
    return (layer_out, next_state)


def solution(mesh):
    return jax.shard_map(
        local,
        mesh=mesh,
        in_specs=(
            P("ep", None),
            P("ep", "tp", None),
            P(),
            P(None, "tp"),
            P(None, "tp"),
            P(None, "tp"),
            P(None, "tp"),
            P("tp"),
            P("tp"),
            P("tp"),
            P("tp"),
            P("tp"),
            P("tp", None),
            P(),
            P(),
            P("ep", None),
            P("ep", None, "tp"),
            P("ep", None, "tp"),
            P("ep", "tp", None),
            P(None, "ep"),
            P(None, "ep"),
            P("ep", None),
            P(),
        ),
        out_specs=(P(("ep", "tp"), None), P("ep", "tp", None)),
        check_vma=False,
    )
```

```python
import functools

import jax
import jax.numpy as jnp
from jax import lax
from jax.experimental import pallas as pl
from jax.experimental.pallas import tpu as pltpu
from jax.sharding import PartitionSpec as P

HEAD_WIDTH = 64
F32 = jnp.float32
BF16 = jnp.bfloat16
MIB = 1 << 20
HIGHEST = lax.Precision.HIGHEST
HBM = pl.BlockSpec(memory_space=pltpu.HBM)
VMEM = pl.BlockSpec(memory_space=pltpu.VMEM)


def iota(shape, dim):
    return lax.broadcasted_iota(jnp.int32, shape, dim)


def dot(a, b):
    return jnp.dot(a, b, preferred_element_type=F32)


def dot_exact(a, b):
    return jnp.dot(a, b, preferred_element_type=F32, precision=HIGHEST)


def halves(x):
    high = x.astype(BF16)
    return high, (x - high.astype(F32)).astype(BF16)


def rms_rows(floats, gain):
    return floats * lax.rsqrt(jnp.mean(floats * floats, axis=-1, keepdims=True) + 1e-06) * gain


def silu(x):
    return x * jax.nn.sigmoid(x)


def attention_kernel(
    tokens,
    gain,
    dec_off,
    cor_off,
    cor_fac,
    own_w,
    head_gain,
    routing,
    weights,
    second_gain,
    state,
    rec_m,
    key_m,
    val_m,
    dec_m,
    out_m,
    *refs,
):
    ahead = refs[: (len(refs) - 17) // 2]
    refs = refs[len(ahead) :]
    next_state, partial, pick, table, tokens_near, gain_near = refs[:6]
    ahead_near = refs[6 : 6 + len(ahead)]
    rows_ref, stage, rec_v, key_v, val_v, dec_v, out_v, mat_sem, in_sem, out_sem, far_sem = refs[
        6 + len(ahead) :
    ]
    seqs, heads, area = state.shape
    width = HEAD_WIDTH
    count = seqs * heads
    chunk = 8 * width
    steps = area // chunk
    mats = [
        pltpu.make_async_copy(source, target, mat_sem.at[n])
        for n, (source, target) in enumerate(
            [(key_m, key_v), (rec_m, rec_v), (val_m, val_v), (dec_m, dec_v), (out_m, out_v)]
        )
    ]
    loads = [
        pltpu.make_async_copy(
            state.at[:, :, pl.ds(j * chunk, chunk)],
            stage.at[:, :, pl.ds(j * chunk, chunk)],
            in_sem.at[j],
        )
        for j in range(steps)
    ]
    stores = [
        pltpu.make_async_copy(
            stage.at[:, :, pl.ds(j * chunk, chunk)],
            next_state.at[:, :, pl.ds(j * chunk, chunk)],
            out_sem.at[j],
        )
        for j in range(steps)
    ]
    fetches = [
        pltpu.make_async_copy(source, target, far_sem.at[n])
        for n, (source, target) in enumerate(zip(ahead, ahead_near))
    ]
    for copy in [*mats[:4], *loads, mats[4], *fetches]:
        copy.start()
    route_tables(routing, weights, pick, table)
    tokens_near[...] = tokens[...]
    gain_near[...] = second_gain[...]
    normed = rms_rows(tokens[...].astype(F32), gain[...]).astype(BF16)
    for copy in mats[:4]:
        copy.wait()
    keys = dot(normed, key_v[...])
    rec = dot(normed, rec_v[...])
    vals = dot(normed, val_v[...])
    decay = jnp.exp(-jnp.exp(dec_off[...] + dot(normed, dec_v[...])))
    rate = jax.nn.sigmoid(cor_off[...] + cor_fac[...] * keys)
    key_in = keys * rate

    def by_head(x):
        return jnp.concatenate([x[:, h * width : (h + 1) * width] for h in range(heads)], axis=0)

    keys_h = by_head(keys)
    unit = (
        keys_h
        * lax.rsqrt(jnp.mean(keys_h * keys_h, axis=-1, keepdims=True) + 1e-06)
        * width ** (-0.5)
    )
    erase = unit * by_head(rate)
    rec_h = by_head(rec)
    key_in_h = by_head(key_in)
    vals_h = by_head(vals)
    decay_h = by_head(decay)
    own = jnp.sum(by_head(rec * key_in * own_w[...]), axis=-1, keepdims=True)
    erase_dot = jnp.sum(erase * rec_h, axis=-1, keepdims=True)
    write_dot = jnp.sum(key_in_h * rec_h, axis=-1, keepdims=True)
    row = iota((count, count), 0)
    col = iota((count, count), 1)
    to_seq = (col == (row % heads) * seqs + row // heads).astype(F32)
    to_head = (row == (col % heads) * seqs + col // heads).astype(F32)
    packed = dot_exact(
        to_seq,
        jnp.concatenate([unit, decay_h * rec_h, decay_h, erase, key_in_h, vals_h], axis=1),
    )

    def twice(n):
        part = packed[:, n * width : (n + 1) * width]
        return jnp.concatenate([part, part], axis=1)

    def wide(n):
        return jnp.concatenate([twice(n)] * (chunk // (2 * width)), axis=1)

    unit_w = wide(0)
    read_w = wide(1)
    sums = jnp.zeros((count, 2 * width), F32)
    lane = iota((chunk, 2 * width), 0) // width
    slot = iota((chunk, 2 * width), 1)
    for j in range(steps):
        part = slice(j * chunk, (j + 1) * chunk)
        loads[j].wait()
        for b in range(seqs):
            rows_ref[b * heads : (b + 1) * heads, part] = stage[b, :, part]
        block = rows_ref[:, part]
        left = (slot == lane + 8 * j).astype(F32).astype(BF16)
        right = (slot == lane + (8 * j + width)).astype(F32).astype(BF16)
        a_hi, a_lo = halves(block * unit_w)
        b_hi, b_lo = halves(block * read_w)
        sums = sums + (dot(a_hi, left) + dot(a_lo, left)) + (dot(b_hi, right) + dot(b_lo, right))
    removed_hi, removed_lo = halves(sums[:, :width])
    removed_x = jnp.concatenate([removed_hi, removed_lo], axis=1)
    vals_hi, vals_lo = halves(packed[:, 5 * width : 6 * width])
    vals_x = jnp.concatenate([vals_hi, vals_lo], axis=1)
    sums_h = dot_exact(to_head, sums)
    read = sums_h[:, width:] - sums_h[:, :width] * erase_dot + vals_h * write_dot
    center = jnp.mean(read, axis=-1, keepdims=True)
    shifted = read - center
    spread_sq = jnp.mean(shifted * shifted, axis=-1, keepdims=True)
    normal = shifted * lax.rsqrt(spread_sq + 0.00064)
    extra = own * vals_h

    def by_lane(x):
        return jnp.concatenate([x[h * seqs : (h + 1) * seqs] for h in range(heads)], axis=1)

    heads_out = (by_lane(normal) * head_gain[...] + by_lane(extra)).astype(BF16)
    mats[4].wait()
    partial[...] = dot(heads_out, out_v[...]).astype(BF16)
    decay_w = wide(2)
    erase_w = wide(3)
    key_w = wide(4)
    source = iota((2 * width, chunk), 0) % width
    target = iota((2 * width, chunk), 1) // width
    for j in range(steps):
        part = slice(j * chunk, (j + 1) * chunk)
        spread = (source == target + 8 * j).astype(F32).astype(BF16)
        rows_ref[:, part] = (
            rows_ref[:, part] * decay_w
            - dot(removed_x, spread) * erase_w
            + dot(vals_x, spread) * key_w
        )
        for b in range(seqs):
            stage[b, :, part] = rows_ref[b * heads : (b + 1) * heads, part]
        stores[j].start()
    for copy in [*fetches, *stores]:
        copy.wait()


def lane_order(seqs):
    per_lane = seqs // lax.axis_size("tp")
    row = iota((seqs, seqs), 0)
    shuffled = ((row // per_lane) ^ lax.axis_index("tp")) * per_lane + row % per_lane
    return (iota((seqs, seqs), 1) == shuffled).astype(F32)


def route_tables(routing, weights, pick, table):
    slots, seqs = pick.shape
    me = lax.axis_index("ep")
    capacity = slots // lax.axis_size("ep")
    slot_row = iota((slots, seqs), 0)
    expert = ((slot_row // capacity) ^ me).astype(F32)
    place_in = (slot_row % capacity).astype(F32)
    every = routing.shape[1]
    mine = iota((every, seqs), 0) == iota((every, seqs), 1) + me * seqs
    routes = dot(routing[...].astype(F32).astype(BF16), mine.astype(F32).astype(BF16))
    chosen = jnp.zeros((slots, seqs), F32)
    weighted = jnp.zeros((slots, seqs), F32)
    for k in range(routing.shape[0]):
        hit = (routes[k : k + 1, :] == expert).astype(F32)
        chosen = chosen + hit
        weighted = weighted + hit * weights[k : k + 1, :]
    earlier = (iota((seqs, seqs), 0) < iota((seqs, seqs), 1)).astype(F32).astype(BF16)
    before = dot(chosen.astype(BF16), earlier)
    here = (before == place_in).astype(F32)
    pick[...] = (chosen * here).astype(BF16)
    table[...] = lax.dot_general(
        lane_order(seqs),
        weighted * here,
        (((1,), (1,)), ((), ())),
        precision=HIGHEST,
        preferred_element_type=F32,
    )


def dispatch_kernel(parts, tokens, gain, pick, own_hidden, *sends):
    seqs, _ = tokens.shape
    groups = len(sends)
    per_lane = own_hidden.shape[0]
    capacity = sends[0].shape[0] - per_lane
    total = parts[0].astype(F32)
    for n in range(1, parts.shape[0]):
        total = total + parts[n].astype(F32)
    hidden = tokens[...].astype(F32) + total
    rows = rms_rows(hidden, gain[...]).astype(BF16)
    sent = dot(pick[...], rows).astype(BF16)
    mine = lane_order(seqs)[:per_lane]
    own_hidden[...] = dot_exact(mine, hidden)
    own_rows = dot(mine.astype(BF16), rows).astype(BF16)
    for send, k in zip(sends, peers(groups)):
        send[:capacity, :] = sent[k * capacity : (k + 1) * capacity]
        send[capacity:, :] = own_rows


def dot_nt(a, b):
    return lax.dot_general(a, b, (((1,), (1,)), ((), ())), preferred_element_type=F32)


def units_kernel(groups, capacity, tile, *refs):
    rows = refs[:groups]
    gate, up, down, dense_gate, dense_up, dense_down = refs[groups : groups + 6]
    outs = refs[groups + 6 : 2 * groups + 6]
    routed, shared = refs[-2:]
    per_lane = rows[0].shape[0] - capacity
    for k in range(groups):
        block = rows[k][...].astype(F32)
        routed[k * capacity : (k + 1) * capacity, :] = block[:capacity]
        shared[k * per_lane : (k + 1) * per_lane, :] = block[capacity:]
    y = shared[...].astype(BF16)
    dense_hidden = (silu(dot_nt(y, dense_gate[...])) * dot_nt(y, dense_up[...])).astype(BF16)
    shared[...] = dot(dense_hidden, dense_down[...])
    x = routed[...].astype(BF16)
    total = jnp.zeros(routed.shape, F32)
    for j in range(gate.shape[2] // tile):
        part = pl.ds(j * tile, tile)
        hidden = (silu(dot(x, gate[0, :, part])) * dot(x, up[0, :, part])).astype(BF16)
        total = total + dot(hidden, down[0, part, :])
    for k in range(groups):
        outs[k][:capacity, :] = total[k * capacity : (k + 1) * capacity].astype(BF16)
        outs[k][capacity:, :] = shared[k * per_lane : (k + 1) * per_lane, :].astype(BF16)


def combine_kernel(groups, table, *refs):
    rows = refs[:groups]
    own, dense = refs[groups : groups + 2]
    sends = refs[groups + 2 : -1]
    gathered = refs[-1]
    per_lane = own.shape[0]
    capacity = rows[0].shape[0] - per_lane
    block = jnp.zeros(own.shape, F32)
    for message, k in zip(rows, peers(groups)):
        values = message[...].astype(F32)
        gathered[k * capacity : (k + 1) * capacity, :] = values[:capacity]
        block = block + values[capacity:]
    dense[...] = block
    x = gathered[...].astype(BF16)
    high, low = halves(table[...])
    result = dot(high, x) + dot(low, x)
    own[...] = result[:per_lane]
    for send, k in zip(sends, peers(len(sends) + 1)[1:]):
        send[...] = result[k * per_lane : (k + 1) * per_lane].astype(BF16)


def final_kernel(hidden, moe, dense, offset, *refs):
    total = moe[...]
    for other in refs[:-1]:
        total = total + other[...].astype(F32)
    out = refs[-1]
    out[...] = (hidden[...] + total + jax.nn.sigmoid(offset[...]) * dense[...]).astype(BF16)


def like(shape, dtype):
    return jax.ShapeDtypeStruct(shape, dtype)


def near(shape, dtype):
    return pltpu.VMEM(shape, dtype)


def far(arrays):
    return [pltpu.with_memory_space_constraint(x, pltpu.HBM) for x in arrays]


def bring(arrays):
    return [pltpu.with_memory_space_constraint(x, pltpu.VMEM) for x in arrays]


def peers(size):
    return sorted(range(size), key=lambda k: -k.bit_length() if k else -size)


def exchange(arrays, axis):
    size = lax.axis_size(axis)
    return [
        lax.ppermute(array, axis, [(i, i ^ k) for i in range(size)]) if k else array
        for k, array in zip(peers(size), arrays)
    ]


def local(
    tokens,
    recurrent_head_state,
    first_norm_gain,
    receptance_matrix,
    key_matrix,
    value_matrix,
    decay_matrix,
    decay_offset,
    correction_offset,
    correction_key_factor,
    own_term_weight,
    head_norm_gain,
    output_matrix,
    second_norm_gain,
    routing,
    routing_weight,
    expert_gate_weight,
    expert_up_weight,
    expert_down_weight,
    dense_gate_weight,
    dense_up_weight,
    dense_down_weight,
    dense_gate_offset,
):
    seqs, width = tokens.shape
    heads, area = recurrent_head_state.shape[1:]
    groups = lax.axis_size("ep")
    lanes = lax.axis_size("tp")
    per_lane = seqs // lanes
    local_experts, _, units = expert_gate_weight.shape
    assert local_experts == 1
    capacity = 2 * seqs * routing.shape[1] // groups

    def row(x):
        return x.reshape(1, -1)

    ahead = []
    steps = area // (8 * HEAD_WIDTH)
    next_state, partial, pick, table, tokens_near, gain_near, *ahead = pl.pallas_call(
        attention_kernel,
        out_shape=(
            like(recurrent_head_state.shape, F32),
            near((seqs, width), BF16),
            near((groups * capacity, seqs), BF16),
            near((seqs, groups * capacity), F32),
            near((seqs, width), BF16),
            near((1, width), F32),
            *[near(x.shape, x.dtype) for x in ahead],
        ),
        in_specs=[VMEM] * 10 + [HBM] * (6 + len(ahead)),
        out_specs=[HBM] + [VMEM] * (5 + len(ahead)),
        scratch_shapes=[
            pltpu.VMEM((seqs * heads, area), F32),
            pltpu.VMEM((seqs, heads, area), F32),
            *[pltpu.VMEM(receptance_matrix.shape, BF16)] * 4,
            pltpu.VMEM(output_matrix.shape, BF16),
            pltpu.SemaphoreType.DMA((5,)),
            pltpu.SemaphoreType.DMA((steps,)),
            pltpu.SemaphoreType.DMA((steps,)),
            pltpu.SemaphoreType.DMA((1,)),
        ],
        compiler_params=pltpu.CompilerParams(vmem_limit_bytes=54 * MIB),
        name="attention",
    )(
        *far(
            [
                tokens,
                row(first_norm_gain),
                row(decay_offset),
                row(correction_offset),
                row(correction_key_factor),
                row(own_term_weight),
                row(head_norm_gain),
                routing.T,
                routing_weight.T,
                row(second_norm_gain),
                recurrent_head_state,
                receptance_matrix,
                key_matrix,
                value_matrix,
                decay_matrix,
                output_matrix,
                *ahead,
            ]
        )
    )
    parts = lax.all_gather(partial, "tp", axis=0, tiled=False)
    message = near((capacity + per_lane, width), BF16)
    own_hidden, *sends = pl.pallas_call(
        dispatch_kernel,
        out_shape=(near((per_lane, width), F32), *[message] * groups),
        in_specs=[VMEM] * 4,
        out_specs=[VMEM] * (1 + groups),
        compiler_params=pltpu.CompilerParams(vmem_limit_bytes=8 * MIB),
        cost_estimate=pl.CostEstimate(flops=20 * 10**9, bytes_accessed=1 << 20, transcendentals=0),
        name="dispatch",
    )(*bring([parts, tokens_near, gain_near, pick]))
    received = exchange(sends, "ep")
    computed = pl.pallas_call(
        functools.partial(units_kernel, groups, capacity, min(256, units)),
        out_shape=[message] * groups,
        in_specs=[VMEM] * (groups + 6),
        out_specs=[VMEM] * groups,
        scratch_shapes=[
            pltpu.VMEM((groups * capacity, width), F32),
            pltpu.VMEM((groups * per_lane, width), F32),
        ],
        compiler_params=pltpu.CompilerParams(vmem_limit_bytes=14 * MIB),
        name="units",
    )(
        *bring(received),
        *bring([expert_gate_weight, expert_up_weight, expert_down_weight]),
        *bring([dense_gate_weight.T, dense_up_weight.T, dense_down_weight]),
    )
    returned = exchange(computed, "ep")
    moe_own, dense_sum, *moe_sends = pl.pallas_call(
        functools.partial(combine_kernel, groups),
        out_shape=[near((per_lane, width), F32)] * 2 + [near((per_lane, width), BF16)] * (lanes - 1),
        in_specs=[VMEM] * (groups + 1),
        out_specs=[VMEM] * (lanes + 1),
        scratch_shapes=[pltpu.VMEM((groups * capacity, width), F32)],
        compiler_params=pltpu.CompilerParams(vmem_limit_bytes=8 * MIB),
        name="combine",
    )(*bring([table, *returned]))
    moe_in = exchange([moe_own] + moe_sends, "tp")
    layer_out = pl.pallas_call(
        final_kernel,
        out_shape=like((per_lane, width), BF16),
        in_specs=[VMEM] * (3 + lanes),
        out_specs=VMEM,
        compiler_params=pltpu.CompilerParams(vmem_limit_bytes=4 * MIB),
        name="final",
    )(*bring([own_hidden, moe_in[0], dense_sum, row(dense_gate_offset), *moe_in[1:]]))
    return (layer_out, next_state)


def solution(mesh):
    return jax.shard_map(
        local,
        mesh=mesh,
        in_specs=(
            P("ep", None),
            P("ep", "tp", None),
            P(),
            P(None, "tp"),
            P(None, "tp"),
            P(None, "tp"),
            P(None, "tp"),
            P("tp"),
            P("tp"),
            P("tp"),
            P("tp"),
            P("tp"),
            P("tp", None),
            P(),
            P(),
            P("ep", None),
            P("ep", None, "tp"),
            P("ep", None, "tp"),
            P("ep", "tp", None),
            P(None, "ep"),
            P(None, "ep"),
            P("ep", None),
            P(),
        ),
        out_specs=(P(("ep", "tp"), None), P("ep", "tp", None)),
        check_vma=False,
    )
```

```python
import functools

import jax
import jax.numpy as jnp
from jax import lax
from jax.experimental import pallas as pl
from jax.experimental.pallas import tpu as pltpu
from jax.sharding import PartitionSpec as P


HEAD_WIDTH = 64
F32 = jnp.float32
BF16 = jnp.bfloat16
MIB = 1 << 20
HIGHEST = lax.Precision.HIGHEST
HBM = pl.BlockSpec(memory_space=pltpu.HBM)
VMEM = pl.BlockSpec(memory_space=pltpu.VMEM)


def iota(shape, dim):
    return lax.broadcasted_iota(jnp.int32, shape, dim)


def dot(a, b):
    return jnp.dot(a, b, preferred_element_type=F32)


def dot_exact(a, b):
    return jnp.dot(a, b, preferred_element_type=F32, precision=HIGHEST)


def halves(x):
    high = x.astype(BF16)
    return high, (x - high.astype(F32)).astype(BF16)


def rms_rows(floats, gain):
    return floats * lax.rsqrt(jnp.mean(floats * floats, axis=-1, keepdims=True) + 1e-06) * gain


def silu(x):
    return x * jax.nn.sigmoid(x)


def attention_kernel(
    tokens,
    gain,
    dec_off,
    cor_off,
    cor_fac,
    own_w,
    head_gain,
    routing,
    weights,
    second_gain,
    state,
    rec_m,
    key_m,
    val_m,
    dec_m,
    out_m,
    *refs,
):
    partial, pick, table, tokens_near, gain_near, rows_ref, packed_ref, removed_ref = refs[:8]
    stage, rec_v, key_v, val_v, dec_v, out_v, mat_sem, in_sem = refs[8:]
    seqs, heads, area = state.shape
    width = HEAD_WIDTH
    count = seqs * heads
    chunk = 8 * width
    steps = area // chunk
    mats = [
        pltpu.make_async_copy(source, target, mat_sem.at[n])
        for n, (source, target) in enumerate(
            [(key_m, key_v), (rec_m, rec_v), (val_m, val_v), (dec_m, dec_v), (out_m, out_v)]
        )
    ]
    loads = [
        pltpu.make_async_copy(
            state.at[:, :, pl.ds(j * chunk, chunk)],
            stage.at[:, :, pl.ds(j * chunk, chunk)],
            in_sem.at[j],
        )
        for j in range(steps)
    ]
    for copy in [*mats[:4], *loads, mats[4]]:
        copy.start()
    route_tables(routing, weights, pick, table)
    tokens_near[...] = tokens[...]
    gain_near[...] = second_gain[...]
    normed = rms_rows(tokens[...].astype(F32), gain[...]).astype(BF16)
    mats[0].wait()
    keys = dot(normed, key_v[...])
    mats[1].wait()
    rec = dot(normed, rec_v[...])
    mats[2].wait()
    vals = dot(normed, val_v[...])
    mats[3].wait()
    decay = jnp.exp(-jnp.exp(dec_off[...] + dot(normed, dec_v[...])))
    rate = jax.nn.sigmoid(cor_off[...] + cor_fac[...] * keys)
    key_in = keys * rate

    def by_head(x):
        return jnp.concatenate([x[:, h * width : (h + 1) * width] for h in range(heads)], axis=0)

    keys_h = by_head(keys)
    unit = (
        keys_h
        * lax.rsqrt(jnp.mean(keys_h * keys_h, axis=-1, keepdims=True) + 1e-06)
        * width ** (-0.5)
    )
    erase = unit * by_head(rate)
    rec_h = by_head(rec)
    key_in_h = by_head(key_in)
    vals_h = by_head(vals)
    decay_h = by_head(decay)
    own = jnp.sum(by_head(rec * key_in * own_w[...]), axis=-1, keepdims=True)
    erase_dot = jnp.sum(erase * rec_h, axis=-1, keepdims=True)
    write_dot = jnp.sum(key_in_h * rec_h, axis=-1, keepdims=True)
    row = iota((count, count), 0)
    col = iota((count, count), 1)
    to_seq = (col == (row % heads) * seqs + row // heads).astype(F32)
    to_head = (row == (col % heads) * seqs + col // heads).astype(F32)
    packed = dot_exact(
        to_seq,
        jnp.concatenate([unit, decay_h * rec_h, decay_h, erase, key_in_h, vals_h], axis=1),
    )

    def twice(n):
        part = packed[:, n * width : (n + 1) * width]
        return jnp.concatenate([part, part], axis=1)

    def wide(n):
        return jnp.concatenate([twice(n)] * (chunk // (2 * width)), axis=1)

    unit_w = wide(0)
    read_w = wide(1)
    sums = jnp.zeros((count, 2 * width), F32)
    lane = iota((chunk, 2 * width), 0) // width
    slot = iota((chunk, 2 * width), 1)
    for j in range(steps):
        part = slice(j * chunk, (j + 1) * chunk)
        loads[j].wait()
        for b in range(seqs):
            rows_ref[b * heads : (b + 1) * heads, part] = stage[b, :, part]
        block = rows_ref[:, part]
        left = (slot == lane + 8 * j).astype(F32).astype(BF16)
        right = (slot == lane + (8 * j + width)).astype(F32).astype(BF16)
        a_hi, a_lo = halves(block * unit_w)
        b_hi, b_lo = halves(block * read_w)
        sums = sums + (dot(a_hi, left) + dot(a_lo, left)) + (dot(b_hi, right) + dot(b_lo, right))
    packed_ref[...] = packed[:, 2 * width :]
    removed_ref[...] = sums
    sums_h = dot_exact(to_head, sums)
    read = sums_h[:, width:] - sums_h[:, :width] * erase_dot + vals_h * write_dot
    center = jnp.mean(read, axis=-1, keepdims=True)
    shifted = read - center
    spread_sq = jnp.mean(shifted * shifted, axis=-1, keepdims=True)
    normal = shifted * lax.rsqrt(spread_sq + 0.00064)
    extra = own * vals_h

    def by_lane(x):
        return jnp.concatenate([x[h * seqs : (h + 1) * seqs] for h in range(heads)], axis=1)

    heads_out = (by_lane(normal) * head_gain[...] + by_lane(extra)).astype(BF16)
    mats[4].wait()
    partial[...] = dot(heads_out, out_v[...]).astype(BF16)


def update_kernel(rows_ref, packed_ref, removed_ref, next_state, stage, out_sem):
    seqs, heads, area = next_state.shape
    width = HEAD_WIDTH
    chunk = 8 * width
    steps = area // chunk
    stores = [
        pltpu.make_async_copy(
            stage.at[:, :, pl.ds(j * chunk, chunk)],
            next_state.at[:, :, pl.ds(j * chunk, chunk)],
            out_sem.at[j],
        )
        for j in range(steps)
    ]
    packed = packed_ref[...]

    def wide(n):
        part = packed[:, n * width : (n + 1) * width]
        return jnp.concatenate([part, part] * (chunk // (2 * width)), axis=1)

    decay_w = wide(0)
    erase_w = wide(1)
    key_w = wide(2)
    removed_hi, removed_lo = halves(removed_ref[:, :width])
    removed_x = jnp.concatenate([removed_hi, removed_lo], axis=1)
    vals_hi, vals_lo = halves(packed[:, 3 * width :])
    vals_x = jnp.concatenate([vals_hi, vals_lo], axis=1)
    source = iota((2 * width, chunk), 0) % width
    target = iota((2 * width, chunk), 1) // width
    for j in range(steps):
        part = slice(j * chunk, (j + 1) * chunk)
        spread = (source == target + 8 * j).astype(F32).astype(BF16)
        block = (
            rows_ref[:, part] * decay_w
            - dot(removed_x, spread) * erase_w
            + dot(vals_x, spread) * key_w
        )
        for b in range(seqs):
            stage[b, :, part] = block[b * heads : (b + 1) * heads]
        stores[j].start()
    for copy in stores:
        copy.wait()


def lane_order(seqs):
    per_lane = seqs // lax.axis_size("tp")
    row = iota((seqs, seqs), 0)
    shuffled = ((row // per_lane) ^ lax.axis_index("tp")) * per_lane + row % per_lane
    return (iota((seqs, seqs), 1) == shuffled).astype(F32)


def route_tables(routing, weights, pick, table):
    slots, seqs = pick.shape
    me = lax.axis_index("ep")
    capacity = slots // lax.axis_size("ep")
    slot_row = iota((slots, seqs), 0)
    expert = ((slot_row // capacity) ^ me).astype(F32)
    place_in = (slot_row % capacity).astype(F32)
    every = routing.shape[1]
    mine = iota((every, seqs), 0) == iota((every, seqs), 1) + me * seqs
    routes = dot(routing[...].astype(F32).astype(BF16), mine.astype(F32).astype(BF16))
    chosen = jnp.zeros((slots, seqs), F32)
    weighted = jnp.zeros((slots, seqs), F32)
    for k in range(routing.shape[0]):
        hit = (routes[k : k + 1, :] == expert).astype(F32)
        chosen = chosen + hit
        weighted = weighted + hit * weights[k : k + 1, :]
    earlier = (iota((seqs, seqs), 0) < iota((seqs, seqs), 1)).astype(F32).astype(BF16)
    before = dot(chosen.astype(BF16), earlier)
    here = (before == place_in).astype(F32)
    pick[...] = (chosen * here).astype(BF16)
    table[...] = lax.dot_general(
        lane_order(seqs),
        weighted * here,
        (((1,), (1,)), ((), ())),
        precision=HIGHEST,
        preferred_element_type=F32,
    )


def dispatch_kernel(lanes, *refs):
    parts = refs[:lanes]
    tokens, gain, pick, own_hidden, own_rows, *sends = refs[lanes:]
    seqs, _ = tokens.shape
    groups = len(sends)
    per_lane = own_hidden.shape[0]
    capacity = sends[0].shape[0]
    total = parts[0][...].astype(F32)
    for part in parts[1:]:
        total = total + part[...].astype(F32)
    hidden = tokens[...].astype(F32) + total
    rows = rms_rows(hidden, gain[...]).astype(BF16)
    sent = dot(pick[...], rows).astype(BF16)
    mine = lane_order(seqs)[:per_lane]
    own_hidden[...] = dot_exact(mine, hidden)
    own_rows[...] = dot(mine.astype(BF16), rows).astype(BF16)
    for send, k in zip(sends, peers(groups)):
        send[...] = sent[k * capacity : (k + 1) * capacity]


def dot_nt(a, b):
    return lax.dot_general(a, b, (((1,), (1,)), ((), ())), preferred_element_type=F32)


def expert_kernel(groups, tile, *refs):
    rows = refs[:groups]
    gate, up, down = refs[groups : groups + 3]
    outs = refs[groups + 3 : 2 * groups + 3]
    routed = refs[-1]
    capacity = rows[0].shape[0]
    for k in range(groups):
        routed[k * capacity : (k + 1) * capacity, :] = rows[k][...].astype(F32)
    x = routed[...].astype(BF16)
    total = jnp.zeros(routed.shape, F32)
    for j in range(gate.shape[2] // tile):
        part = pl.ds(j * tile, tile)
        hidden = (silu(dot(x, gate[0, :, part])) * dot(x, up[0, :, part])).astype(BF16)
        total = total + dot(hidden, down[0, part, :])
    for k in range(groups):
        outs[k][...] = total[k * capacity : (k + 1) * capacity].astype(BF16)


def dense_kernel(groups, *refs):
    rows = refs[:groups]
    gate, up, down = refs[groups : groups + 3]
    outs = refs[groups + 3 : 2 * groups + 3]
    shared = refs[-1]
    per_lane = rows[0].shape[0]
    for k in range(groups):
        shared[k * per_lane : (k + 1) * per_lane, :] = rows[k][...].astype(F32)
    y = shared[...].astype(BF16)
    hidden = (silu(dot_nt(y, gate[...])) * dot_nt(y, up[...])).astype(BF16)
    result = dot(hidden, down[...])
    for k in range(groups):
        outs[k][...] = result[k * per_lane : (k + 1) * per_lane].astype(BF16)


def combine_kernel(groups, table, *refs):
    rows = refs[:groups]
    own = refs[groups]
    sends = refs[groups + 1 : -1]
    gathered = refs[-1]
    per_lane = own.shape[0]
    capacity = rows[0].shape[0]
    for message, k in zip(rows, peers(groups)):
        gathered[k * capacity : (k + 1) * capacity, :] = message[...].astype(F32)
    x = gathered[...].astype(BF16)
    high, low = halves(table[...])
    result = dot(high, x) + dot(low, x)
    own[...] = result[:per_lane]
    for send, k in zip(sends, peers(len(sends) + 1)[1:]):
        send[...] = result[k * per_lane : (k + 1) * per_lane].astype(BF16)


def final_kernel(groups, hidden, moe, offset, *refs):
    total = moe[...]
    for other in refs[:-1 - groups]:
        total = total + other[...].astype(F32)
    blocks = refs[-1 - groups : -1]
    block = blocks[0][...].astype(F32)
    for part in blocks[1:]:
        block = block + part[...].astype(F32)
    out = refs[-1]
    out[...] = (hidden[...] + total + jax.nn.sigmoid(offset[...]) * block).astype(BF16)


def like(shape, dtype):
    return jax.ShapeDtypeStruct(shape, dtype)


def near(shape, dtype):
    return pltpu.VMEM(shape, dtype)


def far(arrays):
    return [pltpu.with_memory_space_constraint(x, pltpu.HBM) for x in arrays]


def bring(arrays):
    return [pltpu.with_memory_space_constraint(x, pltpu.VMEM) for x in arrays]


def peers(size):
    return sorted(range(size), key=lambda k: -k.bit_length() if k else -size)


def exchange(arrays, axis):
    size = lax.axis_size(axis)
    got = []
    for k, array in zip(peers(size), arrays):
        if k:
            array = lax.ppermute(array, axis, [(i, i ^ k) for i in range(size)])
        got.append(array)
    return got


def local(
    tokens,
    recurrent_head_state,
    first_norm_gain,
    receptance_matrix,
    key_matrix,
    value_matrix,
    decay_matrix,
    decay_offset,
    correction_offset,
    correction_key_factor,
    own_term_weight,
    head_norm_gain,
    output_matrix,
    second_norm_gain,
    routing,
    routing_weight,
    expert_gate_weight,
    expert_up_weight,
    expert_down_weight,
    dense_gate_weight,
    dense_up_weight,
    dense_down_weight,
    dense_gate_offset,
):
    seqs, width = tokens.shape
    heads, area = recurrent_head_state.shape[1:]
    groups = lax.axis_size("ep")
    lanes = lax.axis_size("tp")
    per_lane = seqs // lanes
    local_experts, _, units = expert_gate_weight.shape
    assert local_experts == 1
    capacity = 2 * seqs * routing.shape[1] // groups

    def row(x):
        return x.reshape(1, -1)

    steps = area // (8 * HEAD_WIDTH)
    count = seqs * heads
    partial, pick, table, tokens_near, gain_near, rows, packed, removed = pl.pallas_call(
        attention_kernel,
        out_shape=(
            near((seqs, width), BF16),
            near((groups * capacity, seqs), BF16),
            near((seqs, groups * capacity), F32),
            near((seqs, width), BF16),
            near((1, width), F32),
            near((count, area), F32),
            near((count, 4 * HEAD_WIDTH), F32),
            near((count, 2 * HEAD_WIDTH), F32),
        ),
        in_specs=[VMEM] * 10 + [HBM] * 6,
        out_specs=[VMEM] * 8,
        scratch_shapes=[
            pltpu.VMEM((seqs, heads, area), F32),
            *[pltpu.VMEM(receptance_matrix.shape, BF16)] * 4,
            pltpu.VMEM(output_matrix.shape, BF16),
            pltpu.SemaphoreType.DMA((5,)),
            pltpu.SemaphoreType.DMA((steps,)),
        ],
        compiler_params=pltpu.CompilerParams(vmem_limit_bytes=50 * MIB),
        name="attention",
    )(
        *far(
            [
                tokens,
                row(first_norm_gain),
                row(decay_offset),
                row(correction_offset),
                row(correction_key_factor),
                row(own_term_weight),
                row(head_norm_gain),
                routing.T,
                routing_weight.T,
                row(second_norm_gain),
                recurrent_head_state,
                receptance_matrix,
                key_matrix,
                value_matrix,
                decay_matrix,
                output_matrix,
            ]
        )
    )
    parts = exchange([partial] * lanes, "tp")
    next_state = pl.pallas_call(
        update_kernel,
        out_shape=like(recurrent_head_state.shape, F32),
        in_specs=[VMEM] * 3,
        out_specs=HBM,
        scratch_shapes=[
            pltpu.VMEM((seqs, heads, area), F32),
            pltpu.SemaphoreType.DMA((steps,)),
        ],
        compiler_params=pltpu.CompilerParams(vmem_limit_bytes=46 * MIB),
        name="update",
    )(*bring([rows, packed, removed]))
    message = near((capacity, width), BF16)
    shared = near((per_lane, width), BF16)
    own_hidden, own_rows, *sends = pl.pallas_call(
        functools.partial(dispatch_kernel, lanes),
        out_shape=(near((per_lane, width), F32), shared, *[message] * groups),
        in_specs=[VMEM] * (3 + lanes),
        out_specs=[VMEM] * (2 + groups),
        compiler_params=pltpu.CompilerParams(vmem_limit_bytes=8 * MIB),
        cost_estimate=pl.CostEstimate(
            flops=20 * 10**9, bytes_accessed=1 << 20, transcendentals=0
        ),
        name="dispatch",
    )(*bring([*parts, tokens_near, gain_near, pick]))
    received = exchange(sends, "ep")
    shared_rows = exchange([own_rows] * groups, "ep")
    computed = pl.pallas_call(
        functools.partial(expert_kernel, groups, min(256, units)),
        out_shape=[message] * groups,
        in_specs=[VMEM] * (groups + 3),
        out_specs=[VMEM] * groups,
        scratch_shapes=[pltpu.VMEM((groups * capacity, width), F32)],
        compiler_params=pltpu.CompilerParams(vmem_limit_bytes=12 * MIB),
        name="experts",
    )(*bring([*received, expert_gate_weight, expert_up_weight, expert_down_weight]))
    returned = exchange(computed, "ep")
    blocks = pl.pallas_call(
        functools.partial(dense_kernel, groups),
        out_shape=[shared] * groups,
        in_specs=[VMEM] * (groups + 3),
        out_specs=[VMEM] * groups,
        scratch_shapes=[pltpu.VMEM((groups * per_lane, width), F32)],
        compiler_params=pltpu.CompilerParams(vmem_limit_bytes=8 * MIB),
        name="dense",
    )(*bring([*shared_rows, dense_gate_weight.T, dense_up_weight.T, dense_down_weight]))
    blocks = exchange(blocks, "ep")
    moe_own, *moe_sends = pl.pallas_call(
        functools.partial(combine_kernel, groups),
        out_shape=[near((per_lane, width), F32)] + [near((per_lane, width), BF16)] * (lanes - 1),
        in_specs=[VMEM] * (groups + 1),
        out_specs=[VMEM] * lanes,
        scratch_shapes=[pltpu.VMEM((groups * capacity, width), F32)],
        compiler_params=pltpu.CompilerParams(vmem_limit_bytes=8 * MIB),
        name="combine",
    )(*bring([table, *returned]))
    moe_in = exchange([moe_own] + moe_sends, "tp")
    layer_out = pl.pallas_call(
        functools.partial(final_kernel, groups),
        out_shape=like((per_lane, width), BF16),
        in_specs=[VMEM] * (2 + lanes + groups),
        out_specs=VMEM,
        compiler_params=pltpu.CompilerParams(vmem_limit_bytes=4 * MIB),
        name="final",
    )(*bring([own_hidden, moe_in[0], row(dense_gate_offset), *moe_in[1:], *blocks]))
    return (layer_out, next_state)


def solution(mesh):
    return jax.shard_map(
        local,
        mesh=mesh,
        in_specs=(
            P("ep", None),
            P("ep", "tp", None),
            P(),
            P(None, "tp"),
            P(None, "tp"),
            P(None, "tp"),
            P(None, "tp"),
            P("tp"),
            P("tp"),
            P("tp"),
            P("tp"),
            P("tp"),
            P("tp", None),
            P(),
            P(),
            P("ep", None),
            P("ep", None, "tp"),
            P("ep", None, "tp"),
            P("ep", "tp", None),
            P(None, "ep"),
            P(None, "ep"),
            P("ep", None),
            P(),
        ),
        out_specs=(P(("ep", "tp"), None), P("ep", "tp", None)),
        check_vma=False,
    )
```

```python
import functools

import jax
import jax.numpy as jnp
from jax import lax
from jax.experimental import pallas as pl
from jax.experimental.pallas import tpu as pltpu
from jax.sharding import PartitionSpec as P


HEAD_WIDTH = 64
F32 = jnp.float32
BF16 = jnp.bfloat16
MIB = 1 << 20
HIGHEST = lax.Precision.HIGHEST
HBM = pl.BlockSpec(memory_space=pltpu.HBM)
VMEM = pl.BlockSpec(memory_space=pltpu.VMEM)


def iota(shape, dim):
    return lax.broadcasted_iota(jnp.int32, shape, dim)


def dot(a, b):
    return jnp.dot(a, b, preferred_element_type=F32)


def dot_exact(a, b):
    return jnp.dot(a, b, preferred_element_type=F32, precision=HIGHEST)


def halves(x):
    high = x.astype(BF16)
    return high, (x - high.astype(F32)).astype(BF16)


def rms_rows(floats, gain):
    return floats * lax.rsqrt(jnp.mean(floats * floats, axis=-1, keepdims=True) + 1e-06) * gain


def silu(x):
    return x * jax.nn.sigmoid(x)


def attention_kernel(*refs):
    small, large, outs = refs[:10], refs[10:16], refs[16:24]
    stage, rec_v, key_v, val_v, dec_v, out_v, mat_sem, in_sem, small_sem = refs[24:33]
    small_v = refs[33:]
    state, rec_m, key_m, val_m, dec_m, out_m = large
    partial, pick, table, tokens_near, gain_near, rows_ref, packed_ref, removed_ref = outs
    tokens, gain, dec_off, cor_off, cor_fac, own_w, head_gain, routing, weights, second_gain = small_v
    first = [
        pltpu.make_async_copy(source, target, small_sem.at[n])
        for n, (source, target) in enumerate(zip(small, small_v))
    ]
    seqs, heads, area = state.shape
    width = HEAD_WIDTH
    count = seqs * heads
    chunk = 8 * width
    steps = area // chunk
    mats = [
        pltpu.make_async_copy(source, target, mat_sem.at[n])
        for n, (source, target) in enumerate(
            [(key_m, key_v), (rec_m, rec_v), (val_m, val_v), (dec_m, dec_v), (out_m, out_v)]
        )
    ]
    loads = [
        pltpu.make_async_copy(
            state.at[:, :, pl.ds(j * chunk, chunk)],
            stage.at[:, :, pl.ds(j * chunk, chunk)],
            in_sem.at[j],
        )
        for j in range(steps)
    ]
    for copy in [*first, *loads, *mats]:
        copy.start()
    for copy in first:
        copy.wait()
    route_tables(routing, weights, pick, table)
    tokens_near[...] = tokens[...]
    gain_near[...] = second_gain[...]
    normed = rms_rows(tokens[...].astype(F32), gain[...]).astype(BF16)
    for j in range(steps):
        part = slice(j * chunk, (j + 1) * chunk)
        loads[j].wait()
        for b in range(seqs):
            rows_ref[b * heads : (b + 1) * heads, part] = stage[b, :, part]
    mats[0].wait()
    keys = dot(normed, key_v[...])
    mats[1].wait()
    rec = dot(normed, rec_v[...])
    mats[2].wait()
    vals = dot(normed, val_v[...])
    mats[3].wait()
    decay = jnp.exp(-jnp.exp(dec_off[...] + dot(normed, dec_v[...])))
    rate = jax.nn.sigmoid(cor_off[...] + cor_fac[...] * keys)
    key_in = keys * rate

    def by_head(x):
        return jnp.concatenate([x[:, h * width : (h + 1) * width] for h in range(heads)], axis=0)

    keys_h = by_head(keys)
    unit = (
        keys_h
        * lax.rsqrt(jnp.mean(keys_h * keys_h, axis=-1, keepdims=True) + 1e-06)
        * width ** (-0.5)
    )
    erase = unit * by_head(rate)
    rec_h = by_head(rec)
    key_in_h = by_head(key_in)
    vals_h = by_head(vals)
    decay_h = by_head(decay)
    own = jnp.sum(by_head(rec * key_in * own_w[...]), axis=-1, keepdims=True)
    erase_dot = jnp.sum(erase * rec_h, axis=-1, keepdims=True)
    write_dot = jnp.sum(key_in_h * rec_h, axis=-1, keepdims=True)
    row = iota((count, count), 0)
    col = iota((count, count), 1)
    to_seq = (col == (row % heads) * seqs + row // heads).astype(F32)
    to_head = (row == (col % heads) * seqs + col // heads).astype(F32)
    packed = dot_exact(
        to_seq,
        jnp.concatenate([unit, decay_h * rec_h, decay_h, erase, key_in_h, vals_h], axis=1),
    )

    def twice(n):
        part = packed[:, n * width : (n + 1) * width]
        return jnp.concatenate([part, part], axis=1)

    def wide(n):
        return jnp.concatenate([twice(n)] * (chunk // (2 * width)), axis=1)

    unit_w = wide(0)
    read_w = wide(1)
    sums = jnp.zeros((count, 2 * width), F32)
    lane = iota((chunk, 2 * width), 0) // width
    slot = iota((chunk, 2 * width), 1)
    for j in range(steps):
        part = slice(j * chunk, (j + 1) * chunk)
        block = rows_ref[:, part]
        left = (slot == lane + 8 * j).astype(F32).astype(BF16)
        right = (slot == lane + (8 * j + width)).astype(F32).astype(BF16)
        a_hi, a_lo = halves(block * unit_w)
        b_hi, b_lo = halves(block * read_w)
        sums = sums + (dot(a_hi, left) + dot(a_lo, left)) + (dot(b_hi, right) + dot(b_lo, right))
    packed_ref[...] = packed[:, 2 * width :]
    removed_ref[...] = sums
    sums_h = dot_exact(to_head, sums)
    read = sums_h[:, width:] - sums_h[:, :width] * erase_dot + vals_h * write_dot
    center = jnp.mean(read, axis=-1, keepdims=True)
    shifted = read - center
    spread_sq = jnp.mean(shifted * shifted, axis=-1, keepdims=True)
    normal = shifted * lax.rsqrt(spread_sq + 0.00064)
    extra = own * vals_h

    def by_lane(x):
        return jnp.concatenate([x[h * seqs : (h + 1) * seqs] for h in range(heads)], axis=1)

    heads_out = (by_lane(normal) * head_gain[...] + by_lane(extra)).astype(BF16)
    mats[4].wait()
    partial[...] = dot(heads_out, out_v[...]).astype(BF16)


def update_kernel(rows_ref, packed_ref, removed_ref, next_state, stage, out_sem):
    seqs, heads, area = next_state.shape
    width = HEAD_WIDTH
    chunk = 8 * width
    steps = area // chunk
    stores = [
        pltpu.make_async_copy(
            stage.at[:, :, pl.ds(j * chunk, chunk)],
            next_state.at[:, :, pl.ds(j * chunk, chunk)],
            out_sem.at[j],
        )
        for j in range(steps)
    ]
    packed = packed_ref[...]

    def wide(n):
        part = packed[:, n * width : (n + 1) * width]
        return jnp.concatenate([part, part] * (chunk // (2 * width)), axis=1)

    decay_w = wide(0)
    erase_w = wide(1)
    key_w = wide(2)
    removed_hi, removed_lo = halves(removed_ref[:, :width])
    removed_x = jnp.concatenate([removed_hi, removed_lo], axis=1)
    vals_hi, vals_lo = halves(packed[:, 3 * width :])
    vals_x = jnp.concatenate([vals_hi, vals_lo], axis=1)
    source = iota((2 * width, chunk), 0) % width
    target = iota((2 * width, chunk), 1) // width
    for j in range(steps):
        part = slice(j * chunk, (j + 1) * chunk)
        spread = (source == target + 8 * j).astype(F32).astype(BF16)
        block = (
            rows_ref[:, part] * decay_w
            - dot(removed_x, spread) * erase_w
            + dot(vals_x, spread) * key_w
        )
        for b in range(seqs):
            stage[b, :, part] = block[b * heads : (b + 1) * heads]
        stores[j].start()
    for copy in stores:
        copy.wait()


def lane_order(seqs):
    per_lane = seqs // lax.axis_size("tp")
    row = iota((seqs, seqs), 0)
    shuffled = ((row // per_lane) ^ lax.axis_index("tp")) * per_lane + row % per_lane
    return (iota((seqs, seqs), 1) == shuffled).astype(F32)


def route_tables(routing, weights, pick, table):
    slots, seqs = pick.shape
    me = lax.axis_index("ep")
    capacity = slots // lax.axis_size("ep")
    slot_row = iota((slots, seqs), 0)
    expert = ((slot_row // capacity) ^ me).astype(F32)
    place_in = (slot_row % capacity).astype(F32)
    every = routing.shape[1]
    mine = iota((every, seqs), 0) == iota((every, seqs), 1) + me * seqs
    routes = dot(routing[...].astype(F32).astype(BF16), mine.astype(F32).astype(BF16))
    chosen = jnp.zeros((slots, seqs), F32)
    weighted = jnp.zeros((slots, seqs), F32)
    for k in range(routing.shape[0]):
        hit = (routes[k : k + 1, :] == expert).astype(F32)
        chosen = chosen + hit
        weighted = weighted + hit * weights[k : k + 1, :]
    earlier = (iota((seqs, seqs), 0) < iota((seqs, seqs), 1)).astype(F32).astype(BF16)
    before = dot(chosen.astype(BF16), earlier)
    here = (before == place_in).astype(F32)
    pick[...] = (chosen * here).astype(BF16)
    table[...] = lax.dot_general(
        lane_order(seqs),
        weighted * here,
        (((1,), (1,)), ((), ())),
        precision=HIGHEST,
        preferred_element_type=F32,
    )


def dispatch_kernel(lanes, *refs):
    parts = refs[:lanes]
    tokens, gain, pick, own_hidden, own_rows, *sends = refs[lanes:]
    seqs, _ = tokens.shape
    groups = len(sends)
    per_lane = own_hidden.shape[0]
    capacity = sends[0].shape[0]
    total = parts[0][...].astype(F32)
    for part in parts[1:]:
        total = total + part[...].astype(F32)
    hidden = tokens[...].astype(F32) + total
    rows = rms_rows(hidden, gain[...]).astype(BF16)
    sent = dot(pick[...], rows).astype(BF16)
    mine = lane_order(seqs)[:per_lane]
    own_hidden[...] = dot_exact(mine, hidden)
    own_rows[...] = dot(mine.astype(BF16), rows).astype(BF16)
    for send, k in zip(sends, peers(groups)):
        send[...] = sent[k * capacity : (k + 1) * capacity]


def dot_nt(a, b):
    return lax.dot_general(a, b, (((1,), (1,)), ((), ())), preferred_element_type=F32)


def expert_kernel(groups, tile, *refs):
    rows = refs[:groups]
    gate, up, down = refs[groups : groups + 3]
    outs = refs[groups + 3 : 2 * groups + 3]
    routed = refs[-1]
    capacity = rows[0].shape[0]
    for k in range(groups):
        routed[k * capacity : (k + 1) * capacity, :] = rows[k][...].astype(F32)
    x = routed[...].astype(BF16)
    total = jnp.zeros(routed.shape, F32)
    for j in range(gate.shape[2] // tile):
        part = pl.ds(j * tile, tile)
        hidden = (silu(dot(x, gate[0, :, part])) * dot(x, up[0, :, part])).astype(BF16)
        total = total + dot(hidden, down[0, part, :])
    for k in range(groups):
        outs[k][...] = total[k * capacity : (k + 1) * capacity].astype(BF16)


def dense_kernel(groups, *refs):
    rows = refs[:groups]
    gate, up, down = refs[groups : groups + 3]
    outs = refs[groups + 3 : 2 * groups + 3]
    shared = refs[-1]
    per_lane = rows[0].shape[0]
    for k in range(groups):
        shared[k * per_lane : (k + 1) * per_lane, :] = rows[k][...].astype(F32)
    y = shared[...].astype(BF16)
    hidden = (silu(dot_nt(y, gate[...])) * dot_nt(y, up[...])).astype(BF16)
    result = dot(hidden, down[...])
    for k in range(groups):
        outs[k][...] = result[k * per_lane : (k + 1) * per_lane].astype(BF16)


def combine_kernel(groups, table, *refs):
    rows = refs[:groups]
    own = refs[groups]
    sends = refs[groups + 1 : -1]
    gathered = refs[-1]
    per_lane = own.shape[0]
    capacity = rows[0].shape[0]
    for message, k in zip(rows, peers(groups)):
        gathered[k * capacity : (k + 1) * capacity, :] = message[...].astype(F32)
    x = gathered[...].astype(BF16)
    high, low = halves(table[...])
    result = dot(high, x) + dot(low, x)
    own[...] = result[:per_lane]
    for send, k in zip(sends, peers(len(sends) + 1)[1:]):
        send[...] = result[k * per_lane : (k + 1) * per_lane].astype(BF16)


def final_kernel(groups, hidden, moe, offset, *refs):
    total = moe[...]
    for other in refs[:-1 - groups]:
        total = total + other[...].astype(F32)
    blocks = refs[-1 - groups : -1]
    block = blocks[0][...].astype(F32)
    for part in blocks[1:]:
        block = block + part[...].astype(F32)
    out = refs[-1]
    out[...] = (hidden[...] + total + jax.nn.sigmoid(offset[...]) * block).astype(BF16)


def like(shape, dtype):
    return jax.ShapeDtypeStruct(shape, dtype)


def near(shape, dtype):
    return pltpu.VMEM(shape, dtype)


def far(arrays):
    return [pltpu.with_memory_space_constraint(x, pltpu.HBM) for x in arrays]


def bring(arrays):
    return [pltpu.with_memory_space_constraint(x, pltpu.VMEM) for x in arrays]


def peers(size):
    return sorted(range(size), key=lambda k: -k.bit_length() if k else -size)


def exchange(arrays, axis):
    size = lax.axis_size(axis)
    got = []
    for k, array in zip(peers(size), arrays):
        if k:
            array = lax.ppermute(array, axis, [(i, i ^ k) for i in range(size)])
        got.append(array)
    return got


def local(
    tokens,
    recurrent_head_state,
    first_norm_gain,
    receptance_matrix,
    key_matrix,
    value_matrix,
    decay_matrix,
    decay_offset,
    correction_offset,
    correction_key_factor,
    own_term_weight,
    head_norm_gain,
    output_matrix,
    second_norm_gain,
    routing,
    routing_weight,
    expert_gate_weight,
    expert_up_weight,
    expert_down_weight,
    dense_gate_weight,
    dense_up_weight,
    dense_down_weight,
    dense_gate_offset,
):
    seqs, width = tokens.shape
    heads, area = recurrent_head_state.shape[1:]
    groups = lax.axis_size("ep")
    lanes = lax.axis_size("tp")
    per_lane = seqs // lanes
    local_experts, _, units = expert_gate_weight.shape
    assert local_experts == 1
    capacity = 2 * seqs * routing.shape[1] // groups

    def row(x):
        return x.reshape(1, -1)

    steps = area // (8 * HEAD_WIDTH)
    count = seqs * heads
    small = [
        tokens,
        row(first_norm_gain),
        row(decay_offset),
        row(correction_offset),
        row(correction_key_factor),
        row(own_term_weight),
        row(head_norm_gain),
        routing.T,
        routing_weight.T,
        row(second_norm_gain),
    ]
    partial, pick, table, tokens_near, gain_near, rows, packed, removed = pl.pallas_call(
        attention_kernel,
        out_shape=(
            near((seqs, width), BF16),
            near((groups * capacity, seqs), BF16),
            near((seqs, groups * capacity), F32),
            near((seqs, width), BF16),
            near((1, width), F32),
            near((count, area), F32),
            near((count, 4 * HEAD_WIDTH), F32),
            near((count, 2 * HEAD_WIDTH), F32),
        ),
        in_specs=[HBM] * 16,
        out_specs=[VMEM] * 8,
        scratch_shapes=[
            pltpu.VMEM((seqs, heads, area), F32),
            *[pltpu.VMEM(receptance_matrix.shape, BF16)] * 4,
            pltpu.VMEM(output_matrix.shape, BF16),
            pltpu.SemaphoreType.DMA((5,)),
            pltpu.SemaphoreType.DMA((steps,)),
            pltpu.SemaphoreType.DMA((len(small),)),
            *[pltpu.VMEM(x.shape, x.dtype) for x in small],
        ],
        compiler_params=pltpu.CompilerParams(vmem_limit_bytes=50 * MIB),
        name="attention",
    )(
        *far(
            [
                *small,
                recurrent_head_state,
                receptance_matrix,
                key_matrix,
                value_matrix,
                decay_matrix,
                output_matrix,
            ]
        )
    )
    parts = exchange([partial] * lanes, "tp")
    next_state = pl.pallas_call(
        update_kernel,
        out_shape=like(recurrent_head_state.shape, F32),
        in_specs=[VMEM] * 3,
        out_specs=HBM,
        scratch_shapes=[
            pltpu.VMEM((seqs, heads, area), F32),
            pltpu.SemaphoreType.DMA((steps,)),
        ],
        compiler_params=pltpu.CompilerParams(vmem_limit_bytes=46 * MIB),
        name="update",
    )(*bring([rows, packed, removed]))
    message = near((capacity, width), BF16)
    shared = near((per_lane, width), BF16)
    own_hidden, own_rows, *sends = pl.pallas_call(
        functools.partial(dispatch_kernel, lanes),
        out_shape=(near((per_lane, width), F32), shared, *[message] * groups),
        in_specs=[VMEM] * (3 + lanes),
        out_specs=[VMEM] * (2 + groups),
        compiler_params=pltpu.CompilerParams(vmem_limit_bytes=8 * MIB),
        cost_estimate=pl.CostEstimate(
            flops=20 * 10**9, bytes_accessed=1 << 20, transcendentals=0
        ),
        name="dispatch",
    )(*bring([*parts, tokens_near, gain_near, pick]))
    received = exchange(sends, "ep")
    shared_rows = exchange([own_rows] * groups, "ep")
    computed = pl.pallas_call(
        functools.partial(expert_kernel, groups, min(256, units)),
        out_shape=[message] * groups,
        in_specs=[VMEM] * (groups + 3),
        out_specs=[VMEM] * groups,
        scratch_shapes=[pltpu.VMEM((groups * capacity, width), F32)],
        compiler_params=pltpu.CompilerParams(vmem_limit_bytes=12 * MIB),
        name="experts",
    )(*bring([*received, expert_gate_weight, expert_up_weight, expert_down_weight]))
    returned = exchange(computed, "ep")
    blocks = pl.pallas_call(
        functools.partial(dense_kernel, groups),
        out_shape=[shared] * groups,
        in_specs=[VMEM] * (groups + 3),
        out_specs=[VMEM] * groups,
        scratch_shapes=[pltpu.VMEM((groups * per_lane, width), F32)],
        compiler_params=pltpu.CompilerParams(vmem_limit_bytes=8 * MIB),
        name="dense",
    )(*bring([*shared_rows, dense_gate_weight.T, dense_up_weight.T, dense_down_weight]))
    blocks = exchange(blocks, "ep")
    moe_own, *moe_sends = pl.pallas_call(
        functools.partial(combine_kernel, groups),
        out_shape=[near((per_lane, width), F32)] + [near((per_lane, width), BF16)] * (lanes - 1),
        in_specs=[VMEM] * (groups + 1),
        out_specs=[VMEM] * lanes,
        scratch_shapes=[pltpu.VMEM((groups * capacity, width), F32)],
        compiler_params=pltpu.CompilerParams(vmem_limit_bytes=8 * MIB),
        name="combine",
    )(*bring([table, *returned]))
    moe_in = exchange([moe_own] + moe_sends, "tp")
    layer_out = pl.pallas_call(
        functools.partial(final_kernel, groups),
        out_shape=like((per_lane, width), BF16),
        in_specs=[VMEM] * (2 + lanes + groups),
        out_specs=VMEM,
        compiler_params=pltpu.CompilerParams(vmem_limit_bytes=4 * MIB),
        name="final",
    )(*bring([own_hidden, moe_in[0], row(dense_gate_offset), *moe_in[1:], *blocks]))
    return (layer_out, next_state)


def solution(mesh):
    return jax.shard_map(
        local,
        mesh=mesh,
        in_specs=(
            P("ep", None),
            P("ep", "tp", None),
            P(),
            P(None, "tp"),
            P(None, "tp"),
            P(None, "tp"),
            P(None, "tp"),
            P("tp"),
            P("tp"),
            P("tp"),
            P("tp"),
            P("tp"),
            P("tp", None),
            P(),
            P(),
            P("ep", None),
            P("ep", None, "tp"),
            P("ep", None, "tp"),
            P("ep", "tp", None),
            P(None, "ep"),
            P(None, "ep"),
            P("ep", None),
            P(),
        ),
        out_specs=(P(("ep", "tp"), None), P("ep", "tp", None)),
        check_vma=False,
    )
```
